32 devices in a mesh: sp: 8 (over z, x), tp: 4 (over y, core).
Axes of the slice: x: 2, y: 2, z: 4, core: 2. Of those that a mesh axis runs over, the one named last changes fastest.
Arguments:
- mixer_out: bfloat16 [1024, 2048], P('sp', 'tp'), may hold values from -12 to 12
- layer_grad: bfloat16 [1024, 2048], P('sp', 'tp'), may hold values from -6 to 6
- row_scale: float32 [1024], P('sp'), may hold values from 0.3 to 3
- norm_gain: bfloat16 [2048], replicated, may hold values from 0.099609375 to 1.8984375
- routes: int32 [1024, 2], P('sp'), may hold values from 0 to 7, all different within a row; in each aligned block of 128 rows (0 to 127, 128 to 255, ...) at most 64 rows name the same one
- route_weight: float32 [1024, 2], P('sp'), may hold values from 0.05 to 0.35
- expert_gate: bfloat16 [8, 3584, 2048], P('sp', 'tp'), may hold values from -0.125 to 0.125
- expert_up: bfloat16 [8, 3584, 2048], P('sp', 'tp'), may hold values from -0.125 to 0.125
- expert_down: bfloat16 [8, 3584, 2048], P('sp', 'tp'), may hold values from -0.09375 to 0.09375
- query_rows: bfloat16 [1024, 1024], P('sp', 'tp'), may hold values from -6 to 6
- key_rows: bfloat16 [1024, 1024], P('sp', 'tp'), may hold values from -6 to 6
- value_rows: bfloat16 [1024, 1024], P('sp', 'tp'), may hold values from -6 to 6
- retained: bfloat16 [1024, 1024], P('sp', 'tp'), may hold values from -6 to 6
- log_decay: float32 [16, 1024], P('tp', 'sp'), may hold values from -0.8 to 0
- entry_state: float32 [8, 16, 64, 64], P('sp', 'tp'), may hold values from -12 to 12
- out_proj: bfloat16 [1024, 2048], P('tp'), may hold values from -0.1875 to 0.1875
Outputs:
- grad_up: bfloat16 [8, 3584, 2048], P('sp', 'tp')
- grad_down: bfloat16 [8, 3584, 2048], P('sp', 'tp')
- grad_proj: float32 [2048, 1024], P('sp', 'tp')
- grad_query: bfloat16 [1024, 1024], P('sp', 'tp')
- grad_key: bfloat16 [1024, 1024], P('sp', 'tp')
- grad_value: bfloat16 [1024, 1024], P('sp', 'tp')
- stream_grad: bfloat16 [1024, 2048], P('sp', 'tp')
The draws below stay inside these ranges and needn't reach their ends.
Inputs may be any that keep to these rules, and one draw needn't show every extreme that they name: `routes`: each row names 2 different experts. Among the entries of one block of 128 consecutive rows no expert appears more than 64 times, and in every draw some block names some expert exactly 64 times.
All inputs are finite; a program needn't handle non-finite values.
Results may differ from the reference program's by a relative error of at most 0.025.
Values may be sent and summed in bfloat16 or wider, within the bound.
A program may use at most 64 MiB of HBM per device.

```python
import math
import jax
import jax.numpy as jnp
import numpy as np
from jax import lax

D = 2048
FF = 3584
HEADS = 16
HEAD_DIM = 64
TOP = 2
TOK_DEV = 128
TOKENS = 1024
EXPERTS = 8
CAP = 64
RET_W = 1024
N_SP = 8
N_TP = 4


def draw_log_decay(key, part):
    base = jax.random.fold_in(key, 7)
    pick_key, fast_key, slow_key, block_key, rough_key, spot_key, depth_key = jax.random.split(base, 7)
    share = 0.5
    fast = jax.random.uniform(pick_key, (HEADS, 1)) < share
    fast_rate = jnp.exp(jax.random.uniform(fast_key, (HEADS, 1), minval=jnp.log(1.0 / 50.0), maxval=jnp.log(1.0 / 20.0)))
    slow_rate = jnp.exp(jax.random.uniform(slow_key, (HEADS, 1), minval=jnp.log(0.15), maxval=jnp.log(0.5))) / TOKENS
    decay_rate = jnp.where(fast, fast_rate, slow_rate)
    decay_factor = jnp.exp(jax.random.uniform(block_key, (HEADS, TOKENS // TOK_DEV), minval=jnp.log(0.5), maxval=jnp.log(2.0)))
    decay_factor = jnp.repeat(decay_factor, TOK_DEV, axis=1)
    coarse_estimate = jax.random.uniform(rough_key, (HEADS, TOKENS), minval=0.5, maxval=1.5)
    spots = jax.random.randint(spot_key, (HEADS, 2), 0, TOKENS)
    layer_depth_level = jnp.log(jax.random.uniform(depth_key, (HEADS, 2), minval=0.55, maxval=0.8))
    position_index = jnp.arange(TOKENS)[None, :, None] == spots[:, None, :]
    retention_spurt = jnp.sum(jnp.where(position_index, layer_depth_level[:, None, :], 0.0), axis=2)
    return (retention_spurt - decay_rate * decay_factor * coarse_estimate).astype(jnp.float32)


def draw_mixer_out(key, part):
    base = jax.random.fold_in(key, 13)
    value_key = jax.random.fold_in(base, 0)
    ascending_decay = jnp.exp(jnp.linspace(0.0, jnp.log(4.0), D))[None, :]
    value = jax.random.normal(value_key, (TOKENS, D)) * ascending_decay
    return jnp.clip(value, -12.0, 12.0).astype(jnp.bfloat16)


def strengthened(result, own_key, source, target, parts, factor):
    owner, partner = [(jnp.arange(result.shape[dim]) // (result.shape[dim] // parts)).reshape([-1 if axis == dim else 1 for axis in range(result.ndim)]) for dim in (source, target)]
    chosen = jax.random.permutation(own_key, parts)[partner]
    strong = (owner == chosen) | (owner == (partner + parts // 2) % parts)
    return jnp.where(strong, factor * result, result)


def level_of(rng, dims, cuts, smallest, high):
    factor_of, own = 1.0, jax.random.fold_in(rng, 6)
    for axis_at, blocks in cuts:
        draws = jnp.exp(jax.random.uniform(jax.random.fold_in(own, axis_at), (blocks,), jnp.float32, smallest / len(cuts), high / len(cuts)))
        factor_of = factor_of * jnp.repeat(draws, dims[axis_at] // blocks).reshape([-1 if axis == axis_at else 1 for axis in range(len(dims))])
    return factor_of


def routed_block(own_key, own, number, rows, amount, top, most, lean):
    ranking = jax.random.permutation(own_key, amount)
    packed, usual = load_shares(amount, rows * top, most, lean, True), load_shares(amount, rows * top, most, lean, False)
    places = jnp.arange(amount)

    def named(tallies, offset_by):
        used = int((tallies > 0).sum())
        fixed = max(1, used // 4)
        moved = fixed + (places - fixed + offset_by * (used - fixed)) % max(1, amount - fixed)
        return jnp.zeros((amount,), jnp.int32).at[ranking[jnp.where(places < fixed, places, moved)]].set(jnp.asarray(tallies, jnp.int32))

    tallies = jnp.where(number % 4 == 0, named(packed, number // 4), named(usual, number - number // 4 - 1))
    mixed = jax.random.permutation(jax.random.fold_in(own, 3), amount)
    donor, sink = mixed[0:amount // 2 * 2:2], mixed[1:amount // 2 * 2:2]
    room = jnp.minimum(tallies[donor] - 1, most - tallies[sink]) // 2
    room = jnp.where((donor == ranking[0]) | (sink == ranking[0]) | (tallies[sink] == 0), 0, jnp.maximum(room, 0))
    moved = jax.random.randint(jax.random.fold_in(own, 4), (amount // 2,), 0, 1 << 20) % (room + 1)
    tallies = tallies.at[donor].add(-moved).at[sink].add(moved)
    items = jnp.searchsorted(jnp.cumsum(tallies), jnp.arange(rows * top), side="right").astype(jnp.int32)
    table = items.reshape(top, rows).T
    table = table[jax.random.permutation(jax.random.fold_in(own, 1), rows)]
    offset_by = jax.random.randint(jax.random.fold_in(own, 2), (rows, 1), 0, top)
    return jnp.take_along_axis(table, (jnp.arange(top)[None, :] + offset_by) % top, axis=1)


def load_shares(number_of, total, limit, skew, full):
    loads = [(1 << 20) // math.isqrt(rank ** skew) + 1 for rank in range(1, number_of + 1)]
    largest = limit if full else min(limit, max(-(-total // number_of), total * loads[0] // sum(loads)))
    least = 1 if total - largest >= number_of - 1 else 0
    counts, surplus = [largest] + [least] * (number_of - 1), total - largest - least * (number_of - 1)
    while surplus > 0:
        free = [i for i in range(1, number_of) if counts[i] < largest] or [i for i in range(1, number_of) if counts[i] < limit]
        pool, left = sum([loads[i] for i in free]), surplus
        for i in free:
            more = min(limit - counts[i], max(1, left * loads[i] // pool), surplus)
            counts[i] = counts[i] + more
            surplus = surplus - more
    return np.array(counts)


def scatter_about(own_key, dims, scale, bound, shards=(), kind=jnp.bfloat16):
    array = jax.random.normal(own_key, dims, jnp.float32) * scale
    if len(shards) > 0:
        array = level_of(own_key, dims, shards, -0.22, 0.18) * array
    return jnp.clip(array, min=-bound, max=bound).astype(kind)


def noise_with(stream_key, dims, scale, limit, cuts, heavy, held_as=jnp.bfloat16):
    array = scale * jax.random.normal(stream_key, dims, jnp.float32)
    if cuts:
        array = array * level_of(stream_key, dims, cuts, -0.22, 0.18)
    return jnp.clip(strengthened(array, jax.random.fold_in(stream_key, 3), *heavy), -limit, limit).astype(held_as)


def setup_inputs(seed: int = 0) -> dict:
    keys = jax.random.split(jax.random.key(seed), 17)
    mixer_out = draw_mixer_out(jax.random.fold_in(keys[16], 71), 0)
    layer_grad = noise_with(keys[1], (TOKENS, D), 1.0, 6.0, ((0, 8), (1, 4)), (0, 1, 8, 2.0))
    row_scale = jnp.clip(jnp.exp(math.log(3.0) - 2.3025851 * jax.random.uniform(keys[2], (TOKENS,), jnp.float32) ** level_of(keys[2], (TOKENS,), ((0, 8),), -0.2, 0.2)), 0.3, 3.0)
    norm_gain = jnp.clip(1.0 + 0.18 * jax.random.normal(keys[3], (D,), jnp.float32), 0.099609375, 1.8984375).astype(jnp.bfloat16)
    routes_keys = jax.random.split(jax.random.fold_in(keys[4], 1), TOKENS // TOK_DEV)
    routes_turns = jax.random.permutation(jax.random.fold_in(keys[4], 3), TOKENS // TOK_DEV)
    routes = jax.vmap(lambda own, number: routed_block(jax.random.fold_in(keys[4], 2), own, number, TOK_DEV, EXPERTS, TOP, CAP, 1))(routes_keys, routes_turns).reshape((TOKENS, TOP))
    route_weight = jnp.clip(0.05 + 0.29999999 * jax.random.uniform(keys[5], (TOKENS, TOP), jnp.float32) ** level_of(keys[5], (TOKENS, TOP), ((0, 8),), -0.2, 0.2), 0.05, 0.35)
    expert_gate = scatter_about(keys[6], (EXPERTS, FF, D), D ** -0.5, 0.125, ((0, 8), (1, 4)))
    expert_up = scatter_about(keys[7], (EXPERTS, FF, D), D ** -0.5, 0.125, ((0, 8), (1, 4)))
    expert_down = scatter_about(keys[8], (EXPERTS, FF, D), FF ** -0.5, 0.09375, ((0, 8), (1, 4)))
    query_rows = scatter_about(keys[9], (TOKENS, RET_W), 1.0, 6.0, ((0, 8), (1, 4)))
    key_rows = scatter_about(keys[10], (TOKENS, RET_W), 1.0, 6.0, ((0, 8), (1, 4)))
    value_rows = scatter_about(keys[11], (TOKENS, RET_W), 1.0, 6.0, ((0, 8), (1, 4)))
    retained = scatter_about(keys[12], (TOKENS, RET_W), 1.0, 6.0, ((0, 8), (1, 4)))
    log_decay = draw_log_decay(jax.random.fold_in(keys[16], 71), 0)
    entry_state = scatter_about(keys[14], (N_SP, HEADS, HEAD_DIM, HEAD_DIM), 2.0, 12.0, ((0, 8), (1, 4)), jnp.float32)
    out_proj = scatter_about(keys[15], (RET_W, D), RET_W ** -0.5, 0.1875, ((0, 4),))
    return dict(mixer_out=mixer_out, layer_grad=layer_grad, row_scale=row_scale, norm_gain=norm_gain, routes=routes, route_weight=route_weight, expert_gate=expert_gate, expert_up=expert_up, expert_down=expert_down, query_rows=query_rows, key_rows=key_rows, value_rows=value_rows, retained=retained, log_decay=log_decay, entry_state=entry_state, out_proj=out_proj)


def span_terms(head_queries, head_keys, head_values, head_gradient, decay_head, incoming_state):
    scale = head_queries.shape[-1] ** -0.5
    length = decay_head.shape[1]
    cumul = jnp.cumsum(decay_head, axis=1)
    places = jnp.arange(length)
    causal = (places[:, None] >= places[None, :])[None, :, :]
    spread = cumul[:, :, None] - cumul[:, None, :]
    weights = jnp.where(causal, jnp.exp(jnp.where(causal, spread, 0.0)), 0.0)
    scores = scale * jnp.einsum("thd,shd->hts", head_queries, head_keys, precision=lax.Precision.HIGHEST) * weights
    pressure = scale * jnp.einsum("thd,shd->hts", head_gradient, head_values, precision=lax.Precision.HIGHEST) * weights
    grad_query = jnp.einsum("hts,shd->thd", pressure, head_keys, precision=lax.Precision.HIGHEST)
    grad_key = jnp.einsum("hts,thd->shd", pressure, head_queries, precision=lax.Precision.HIGHEST)
    grad_value = jnp.einsum("hts,thd->shd", scores, head_gradient, precision=lax.Precision.HIGHEST)
    ascending_decay = jnp.exp(cumul).T
    grad_query = grad_query + scale * ascending_decay[:, :, None] * jnp.einsum(
        "joy,oiy->joi", head_gradient, incoming_state, precision=lax.Precision.HIGHEST)
    state_update = jnp.einsum("olb,oli->lbi", head_queries * ascending_decay[:, :, None], head_gradient, precision=lax.Precision.HIGHEST)
    survive = jnp.exp(cumul[:, -1])
    falling = jnp.exp(cumul[:, -1:] - cumul).T
    return grad_query, grad_key, grad_value, state_update, survive, falling


def add_carried(grad_key, grad_value, head_keys, head_values, falling, carried_over_state):
    scale = head_keys.shape[-1] ** -0.5
    grad_key = grad_key + scale * falling[:, :, None] * jnp.einsum(
        "upy,ruy->rup", carried_over_state, head_values, precision=lax.Precision.HIGHEST)
    grad_value = grad_value + scale * falling[:, :, None] * jnp.einsum(
        "rzw,erz->erw", carried_over_state, head_keys, precision=lax.Precision.HIGHEST)
    return grad_key, grad_value


def reference(mixer_out, layer_grad, row_scale, norm_gain, routes, route_weight, expert_gate, expert_up,
              expert_down, query_rows, key_rows, value_rows, retained, log_decay, entry_state, out_proj):
    scaled = mixer_out.astype(jnp.float32) * row_scale[:, None]
    gain_all = norm_gain.astype(jnp.float32)
    normed = (scaled * gain_all[None, :]).astype(jnp.bfloat16)
    weighted = (route_weight[:, :, None] * layer_grad.astype(jnp.float32)[:, None, :]).astype(jnp.bfloat16)
    flat_normed = jnp.concatenate([jnp.repeat(normed, TOP, axis=0), jnp.zeros((1, D), jnp.bfloat16)], axis=0)
    flat_grad = jnp.concatenate([weighted.reshape(TOKENS * TOP, D), jnp.zeros((1, D), jnp.bfloat16)], axis=0)

    blocks = routes.reshape(N_SP, TOP * TOK_DEV)
    onehot = (blocks[:, :, None] == jnp.arange(EXPERTS, dtype=jnp.int32)[None, None, :]).astype(jnp.int32)
    rank_in = jnp.sum(onehot * (jnp.cumsum(onehot, axis=1) - 1), axis=2)
    source_ids = jnp.arange(N_SP, dtype=jnp.int32)[:, None]
    position = (blocks * (N_SP * CAP) + source_ids * CAP + rank_in).reshape(-1).astype(jnp.int32)
    table = jnp.full((EXPERTS * N_SP * CAP,), TOP * TOKENS, jnp.int32)
    table = table.at[position].set(jnp.arange(TOP * TOKENS, dtype=jnp.int32)).reshape(EXPERTS, N_SP * CAP)

    width = FF // N_TP

    def expert(inputs):
        row_ids, gate_weight, up_weight, down_weight = inputs
        normed_rows = jnp.take(flat_normed, row_ids, axis=0)
        grad_rows = jnp.take(flat_grad, row_ids, axis=0)
        gate_pre = jnp.dot(normed_rows, gate_weight.T, preferred_element_type=jnp.float32)
        up_pre = jnp.dot(normed_rows, up_weight.T, preferred_element_type=jnp.float32)
        sigmoid_gate = jax.nn.sigmoid(gate_pre)
        silu_gate = gate_pre * sigmoid_gate
        activation = (silu_gate * up_pre).astype(jnp.bfloat16)
        grad_down = jnp.dot(activation.T, grad_rows, preferred_element_type=jnp.float32).astype(jnp.bfloat16)
        act_grad = jnp.dot(grad_rows, down_weight.T, preferred_element_type=jnp.float32)
        up_grad = (act_grad * silu_gate).astype(jnp.bfloat16)
        gate_grad = (act_grad * up_pre * sigmoid_gate * (1.0 + gate_pre * (1.0 - sigmoid_gate))).astype(jnp.bfloat16)
        grad_up = jnp.dot(up_grad.T, normed_rows, preferred_element_type=jnp.float32).astype(jnp.bfloat16)

        def group(index, total):
            start = (index * width).astype(jnp.int32)
            part = jnp.dot(lax.dynamic_slice_in_dim(gate_grad, start, width, 1),
                           lax.dynamic_slice_in_dim(gate_weight, start, width, 0),
                           preferred_element_type=jnp.float32)
            part = part + jnp.dot(lax.dynamic_slice_in_dim(up_grad, start, width, 1),
                                  lax.dynamic_slice_in_dim(up_weight, start, width, 0),
                                  preferred_element_type=jnp.float32)
            return total + lax.optimization_barrier(part.astype(jnp.bfloat16)).astype(jnp.float32)

        summed = lax.fori_loop(0, N_TP, group, jnp.zeros((N_SP * CAP, D), jnp.float32))
        return grad_up, grad_down, summed.astype(jnp.bfloat16)

    grad_up, grad_down, returned = lax.map(expert, (table, expert_gate, expert_up, expert_down))
    per_route = jnp.take(returned.reshape(EXPERTS * N_SP * CAP, D), position, axis=0)
    hidden_grad = jnp.sum(per_route.reshape(TOKENS, TOP, D).astype(jnp.float32), axis=1).astype(jnp.bfloat16)

    attend = gain_all[None, :] * hidden_grad.astype(jnp.float32)
    mean_dot = jnp.mean(scaled * attend, axis=1, keepdims=True)
    stream = layer_grad.astype(jnp.float32) + row_scale[:, None] * (attend - scaled * mean_dot)
    stream_grad = stream.astype(jnp.bfloat16)
    grad_proj = jnp.dot(stream_grad.T, retained, preferred_element_type=jnp.float32)
    out_grad = jnp.dot(stream_grad, out_proj.T, preferred_element_type=jnp.float32).astype(jnp.bfloat16)

    def split_heads(block):
        return block.astype(jnp.float32).reshape(N_SP, TOK_DEV, HEADS, HEAD_DIM)

    decay_spans = log_decay.reshape(HEADS, N_SP, TOK_DEV).transpose(1, 0, 2)

    def span_step(carried_over_state, pieces):
        head_queries, head_keys, head_values, head_gradient, decay_head, incoming_state = pieces
        grad_query, grad_key, grad_value, state_update, survive, falling = span_terms(
            head_queries, head_keys, head_values, head_gradient, decay_head, incoming_state)
        grad_key, grad_value = add_carried(grad_key, grad_value, head_keys, head_values, falling, carried_over_state)
        return state_update + survive[:, None, None] * carried_over_state, (grad_query, grad_key, grad_value)

    start_state = jnp.zeros((HEADS, HEAD_DIM, HEAD_DIM), jnp.float32)
    _, (grad_query, grad_key, grad_value) = lax.scan(
        span_step, start_state,
        (split_heads(query_rows), split_heads(key_rows), split_heads(value_rows), split_heads(out_grad),
         decay_spans, entry_state), reverse=True)
    ret_width = HEADS * HEAD_DIM
    return (grad_up, grad_down, grad_proj,
            grad_query.reshape(TOKENS, ret_width).astype(jnp.bfloat16),
            grad_key.reshape(TOKENS, ret_width).astype(jnp.bfloat16),
            grad_value.reshape(TOKENS, ret_width).astype(jnp.bfloat16),
            stream_grad)
```

```python
import functools

import jax
import jax.numpy as jnp
from jax import lax
from jax.experimental import pallas as pl
from jax.experimental.pallas import tpu as pltpu
from jax.sharding import PartitionSpec as P

MESH = pl.DeviceIdType.MESH
VMEM = pl.BlockSpec(memory_space=pltpu.VMEM)
BF16, F32 = jnp.bfloat16, jnp.float32


def remote(src, dst, send_sem, recv_sem, device):
    return pltpu.make_async_remote_copy(
        src_ref=src, dst_ref=dst, send_sem=send_sem, recv_sem=recv_sem,
        device_id=device, device_id_type=MESH,
    )


def greet(devices):
    barrier = pltpu.get_barrier_semaphore()
    for device in devices:
        pl.semaphore_signal(barrier, inc=1, device_id=device, device_id_type=MESH)
    pl.semaphore_wait(barrier, len(devices))


class Place:
    def __init__(self, n, tp):
        self.n, self.tp, self.rows = n, tp, tp // 2
        self.s, self.t = lax.axis_index("sp"), lax.axis_index("tp")
        self.core, self.y = lax.rem(self.t, 2), self.t // 2
        self.twin_t = self.t + 1 - 2 * self.core
        self.twin = (self.s, self.twin_t)

    def to_sp(self, k):
        return lax.rem(self.s + k, self.n)

    def from_sp(self, k):
        return lax.rem(self.s + self.n - k, self.n)

    def to_y(self, k):
        return 2 * lax.rem(self.y + k, self.rows) + self.core

    def from_y(self, k):
        return 2 * lax.rem(self.y + self.rows - k, self.rows) + self.core

    def sp_peers(self):
        return [(self.to_sp(k), self.t) for k in range(1, self.n)]

    def tp_peers(self):
        return [(self.s, lax.rem(self.t + k, self.tp)) for k in range(1, self.tp)]

    def y_peers(self):
        return [(self.s, self.to_y(k)) for k in range(1, self.rows)] + [self.twin]


def dispatch_kernel(n, tp, normed_ref, grad_ref, full_n_ref, full_g_ref, buf, s1, r1, s2, r2, s3, r3):
    at = Place(n, tp)
    capacity, columns = normed_ref.shape[1:]
    greet(at.sp_peers() + at.y_peers())
    inputs = (normed_ref, grad_ref)
    pending = []

    def start(copy):
        copy.start()
        pending.append(copy)

    def spread(kind, source, block):
        for k in range(1, at.rows):
            start(remote(block, buf.at[kind, at.t, source], s2.at[kind, k - 1, source],
                         r2.at[kind, k - 1, source], (at.s, at.to_y(k))))
        start(remote(block, buf.at[kind, at.t, source], s3.at[kind, 0, source],
                     r3.at[kind, 0, source], at.twin))

    def hand_on(kind, source):
        for k in range(1, at.rows):
            slot = buf.at[kind, at.from_y(k), source]
            remote(slot, slot, s2.at[kind, k - 1, source], r2.at[kind, k - 1, source], at.twin).wait_recv()
            start(remote(slot, slot, s3.at[kind, k, source], r3.at[kind, k, source], at.twin))

    for kind in range(2):
        spread(kind, at.s, inputs[kind].at[at.s])
        for k in range(1, n):
            there = at.to_sp(k)
            start(remote(inputs[kind].at[there], buf.at[kind, at.t, at.s], s1.at[kind, there],
                         r1.at[kind, at.s], (there, at.t)))
        buf[kind, at.t, at.s] = inputs[kind][at.s]
    lag = [(kind, at.s) for kind in range(2)]
    for kind in range(2):
        for k in range(1, n):
            source = at.from_sp(k)
            slot = buf.at[kind, at.t, source]
            remote(slot, slot, s1.at[kind, source], r1.at[kind, source], at.twin).wait_recv()
            spread(kind, source, slot)
            lag.append((kind, source))
            if len(lag) > 3:
                hand_on(*lag.pop(0))
    for item in lag:
        hand_on(*item)
    for kind in range(2):
        for k in range(n):
            source = at.from_sp(k)
            for hop in range(at.rows):
                owner = at.twin_t if hop == 0 else lax.rem(at.from_y(hop) + 1 - 2 * at.core, tp)
                slot = buf.at[kind, owner, source]
                remote(slot, slot, s3.at[kind, hop, source], r3.at[kind, hop, source], at.twin).wait_recv()
    for kind, out in enumerate((full_n_ref, full_g_ref)):
        for t in range(tp):
            out[:, t * columns:(t + 1) * columns] = buf[kind, t].reshape(n * capacity, columns)
    for copy in pending:
        copy.wait_send()


def dispatch(n, tp, send_normed, send_grad):
    _, capacity, columns = send_normed.shape
    rows = tp // 2
    full = jax.ShapeDtypeStruct((n * capacity, tp * columns), BF16)
    dma = pltpu.SemaphoreType.DMA
    return pl.pallas_call(
        functools.partial(dispatch_kernel, n, tp),
        out_shape=(full, full),
        in_specs=[VMEM] * 2,
        out_specs=(VMEM, VMEM),
        scratch_shapes=[
            pltpu.VMEM((2, tp, n, capacity, columns), BF16),
            dma((2, n)), dma((2, n)),
            dma((2, rows, n)), dma((2, rows, n)),
            dma((2, rows, n)), dma((2, rows, n)),
        ],
        compiler_params=pltpu.CompilerParams(collective_id=1, has_side_effects=True),
        name="dispatch",
    )(send_normed, send_grad)


def eye(size):
    return lax.broadcasted_iota(jnp.int32, (size, size), 0) == lax.broadcasted_iota(jnp.int32, (size, size), 1)


def return_kernel(n, tp, part_ref, pick_ref, mixer_ref, layer_ref, scale_ref, gain_ref, kept_ref, surv_ref,
                  stream_ref, full_ref, kept_all_ref, surv_all_ref,
                  b1, s1buf, b2, total, back, stat, sbuf,
                  sa, ra, sb, rb, sc, rc, sd, rd, se, re, sf, rf, sk, rk, sv, rv):
    at = Place(n, tp)
    tokens, columns = mixer_ref.shape
    capacity = back.shape[1]
    pair = at.s + 1 - 2 * lax.rem(at.s, 2)
    greet(at.sp_peers() + at.tp_peers())
    pending = []

    def start(copy):
        copy.start()
        pending.append(copy)

    for k in range(at.rows):
        yy = lax.rem(at.y + k, at.rows)
        cols = pl.ds(pl.multiple_of((2 * yy + 1 - at.core) * columns, 128), columns)
        start(remote(part_ref.at[:, cols], b1.at[yy], sa.at[yy], ra.at[yy], at.twin))
    for k in range(1, n):
        there = at.to_sp(k)
        start(remote(surv_ref, surv_all_ref.at[at.s], sv.at[there], rv.at[at.s], (there, at.t)))
    surv_all_ref[at.s] = surv_ref[...]
    for k in range(2, n, 2):
        there = at.to_sp(k)
        start(remote(kept_ref, kept_all_ref.at[at.s], sk.at[0, there], rk.at[at.s], (there, at.t)))
    start(remote(kept_ref, kept_all_ref.at[at.s], sk.at[1, at.s], rk.at[at.s], (pair, at.t)))
    kept_all_ref[at.s] = kept_ref[...]

    for k in range(at.rows):
        yy = lax.rem(at.y + k, at.rows)
        remote(b1.at[yy], b1.at[yy], sa.at[yy], ra.at[yy], at.twin).wait_recv()
    order = [at.to_sp(k) for k in range(1, n)] + [at.s]

    def rows_of(block):
        return pl.ds(pl.multiple_of(block * capacity, capacity), capacity)

    def mine(block, yy):
        cols = pl.ds(pl.multiple_of((2 * yy + at.core) * columns, 128), columns)
        return part_ref[rows_of(block), cols].astype(F32) + b1[yy, rows_of(block), :].astype(F32)

    for block in order:
        for k in range(1, at.rows):
            yy = lax.rem(at.y + k, at.rows)
            s1buf[k - 1, block] = mine(block, yy).astype(BF16)
            start(remote(s1buf.at[k - 1, block], b2.at[k - 1, block], sb.at[k - 1, block],
                         rb.at[k - 1, block], (at.s, at.to_y(k))))
    for place, block in enumerate(order):
        summed = mine(block, at.y)
        for k in range(1, at.rows):
            slot = b2.at[k - 1, block]
            remote(slot, slot, sb.at[k - 1, block], rb.at[k - 1, block], at.twin).wait_recv()
            summed = summed + b2[k - 1, block].astype(F32)
        if place < n - 1:
            total[block] = summed.astype(BF16)
            start(remote(total.at[block], back.at[at.s], sc.at[block], rc.at[at.s], (block, at.t)))
        else:
            back[at.s] = summed.astype(BF16)
    for k in range(2, n, 2):
        source = at.from_sp(k)
        slot = kept_all_ref.at[source]
        remote(slot, slot, sk.at[0, source], rk.at[source], at.twin).wait_recv()
        start(remote(slot, slot, sk.at[1, source], rk.at[source], (pair, at.t)))
    for k in range(1, n):
        source = at.from_sp(k)
        slot = back.at[source]
        remote(slot, slot, sc.at[source], rc.at[source], at.twin).wait_recv()
    hidden = jnp.dot(pick_ref[...], back[...].reshape(n * capacity, columns), preferred_element_type=F32)
    attend = gain_ref[...] * hidden.astype(BF16).astype(F32)
    row_scale = scale_ref[:, 0:1]
    scaled = mixer_ref[...].astype(F32) * row_scale
    column = jnp.sum(scaled * attend, axis=1, keepdims=True)
    diagonal = eye(tokens)
    row = jnp.sum(jnp.where(diagonal, column, 0.0), axis=0, keepdims=True)
    stat[at.t] = jnp.broadcast_to(row, (8, tokens))
    for k in range(1, tp):
        there = lax.rem(at.t + k, tp)
        start(remote(stat.at[at.t], stat.at[at.t], sd.at[there], rd.at[at.t], (at.s, there)))
    for k in range(1, tp):
        source = lax.rem(at.t + tp - k, tp)
        remote(stat.at[source], stat.at[source], sd.at[source], rd.at[source], at.twin).wait_recv()
    summed_row = jnp.sum(stat[...], axis=0)[0:1, :]
    mean_dot = jnp.sum(jnp.where(diagonal, summed_row, 0.0), axis=1, keepdims=True) / (columns * tp)
    stream = (layer_ref[...].astype(F32) + row_scale * (attend - scaled * mean_dot)).astype(BF16)
    stream_ref[...] = stream
    sbuf[at.t] = stream
    for k in range(1, at.rows):
        start(remote(sbuf.at[at.t], sbuf.at[at.t], se.at[k - 1], re.at[k - 1], (at.s, at.to_y(k))))
    start(remote(sbuf.at[at.t], sbuf.at[at.t], sf.at[0], rf.at[0], at.twin))
    for k in range(1, at.rows):
        slot = sbuf.at[at.from_y(k)]
        remote(slot, slot, se.at[k - 1], re.at[k - 1], at.twin).wait_recv()
        start(remote(slot, slot, sf.at[k], rf.at[k], at.twin))
    for hop in range(at.rows):
        owner = at.twin_t if hop == 0 else lax.rem(at.from_y(hop) + 1 - 2 * at.core, tp)
        slot = sbuf.at[owner]
        remote(slot, slot, sf.at[hop], rf.at[hop], at.twin).wait_recv()
    for t in range(tp):
        full_ref[:, t * columns:(t + 1) * columns] = sbuf[t]
    for k in range(1, n):
        source = at.from_sp(k)
        slot = surv_all_ref.at[source]
        remote(slot, slot, sv.at[source], rv.at[source], at.twin).wait_recv()
    for k in range(0, n, 2):
        source = lax.rem(pair + n - k, n)
        slot = kept_all_ref.at[source]
        remote(slot, slot, sk.at[0, source], rk.at[source], at.twin).wait_recv()
    for copy in pending:
        copy.wait_send()


def give_back(n, tp, part, pick, mixer, layer, row_scale, gain, kept, surv):
    tokens, columns = mixer.shape
    rows, capacity = tp // 2, part.shape[0] // n
    dma = pltpu.SemaphoreType.DMA
    return pl.pallas_call(
        functools.partial(return_kernel, n, tp),
        out_shape=(
            jax.ShapeDtypeStruct((tokens, columns), BF16),
            jax.ShapeDtypeStruct((tokens, tp * columns), BF16),
            jax.ShapeDtypeStruct((n,) + kept.shape, BF16),
            jax.ShapeDtypeStruct((n,) + surv.shape, F32),
        ),
        in_specs=[VMEM] * 8,
        out_specs=(VMEM,) * 4,
        scratch_shapes=[
            pltpu.VMEM((rows, n * capacity, columns), BF16),
            pltpu.VMEM((rows, n, capacity, columns), BF16),
            pltpu.VMEM((rows, n, capacity, columns), BF16),
            pltpu.VMEM((n, capacity, columns), BF16),
            pltpu.VMEM((n, capacity, columns), BF16),
            pltpu.VMEM((tp, 8, tokens), F32),
            pltpu.VMEM((tp, tokens, columns), BF16),
            dma((rows,)), dma((rows,)),
            dma((rows, n)), dma((rows, n)),
            dma((n,)), dma((n,)),
            dma((tp,)), dma((tp,)),
            dma((rows,)), dma((rows,)),
            dma((rows,)), dma((rows,)),
            dma((2, n)), dma((n,)),
            dma((n,)), dma((n,)),
        ],
        compiler_params=pltpu.CompilerParams(collective_id=2, has_side_effects=True),
        name="give_back",
    )(part, pick, mixer, layer, row_scale, gain, kept, surv)


def exchange_kernel(n, tp, state_ref, weight_ref, cut_ref, carried_ref, cols_ref, sbuf, cbuf, su, ru, sc, rc, sd, rd):
    at = Place(n, tp)
    tokens = cut_ref.shape[1]
    half = tokens // 2
    greet(at.sp_peers() + [at.twin])
    pending = []

    def start(copy):
        copy.start()
        pending.append(copy)

    own = pl.ds(pl.multiple_of(at.core * half, half), half)
    other = pl.ds(pl.multiple_of((1 - at.core) * half, half), half)
    for k in range(1, n):
        there = at.to_sp(k)
        start(remote(state_ref, sbuf.at[at.s], su.at[there], ru.at[at.s], (there, at.t)))
        start(remote(cut_ref.at[there, own], cbuf.at[at.s, own], sc.at[there], rc.at[at.s], (there, at.t)))
    sbuf[at.s] = state_ref[...]
    cbuf[at.s] = cut_ref[at.s]
    for k in range(1, n):
        source = at.from_sp(k)
        slot = cbuf.at[source, own]
        remote(slot, slot, sc.at[source], rc.at[source], at.twin).wait_recv()
        start(remote(slot, slot, sd.at[source], rd.at[source], at.twin))
    total = jnp.zeros(carried_ref.shape, F32)
    for k in range(1, n):
        source = at.from_sp(k)
        slot = sbuf.at[source]
        remote(slot, slot, su.at[source], ru.at[source], at.twin).wait_recv()
        total = total + weight_ref[source] * sbuf[source].astype(F32)
    carried_ref[...] = total
    for k in range(1, n):
        source = at.from_sp(k)
        slot = cbuf.at[source, other]
        remote(slot, slot, sd.at[source], rd.at[source], at.twin).wait_recv()
    cols_ref[...] = cbuf[...]
    for copy in pending:
        copy.wait_send()


def exchange(n, tp, state, weight, cut):
    dma = pltpu.SemaphoreType.DMA
    return pl.pallas_call(
        functools.partial(exchange_kernel, n, tp),
        out_shape=(jax.ShapeDtypeStruct(state.shape, F32), jax.ShapeDtypeStruct(cut.shape, BF16)),
        in_specs=[VMEM] * 3,
        out_specs=(VMEM, VMEM),
        scratch_shapes=[
            pltpu.VMEM((n,) + state.shape, BF16),
            pltpu.VMEM(cut.shape, BF16),
            dma((n,)), dma((n,)), dma((n,)), dma((n,)), dma((n,)), dma((n,)),
        ],
        compiler_params=pltpu.CompilerParams(collective_id=3, has_side_effects=True),
        name="exchange",
    )(state, weight, cut)


def contract_last(first_op, second_op):
    return lax.dot_general(
        first_op, second_op, (((1,), (1,)), ((), ())), preferred_element_type=jnp.float32
    )


def contract_first(first_op, second_op):
    return lax.dot_general(
        first_op, second_op, (((0,), (0,)), ((), ())), preferred_element_type=jnp.float32
    )


def span_terms(head_queries, head_keys, head_values, head_gradient, decay_head, incoming_state):
    scale = head_queries.shape[-1] ** (-0.5)
    length = decay_head.shape[1]
    cumul = jnp.cumsum(decay_head, axis=1)
    places = jnp.arange(length)
    causal = (places[:, None] >= places[None, :])[None, :, :]
    spread = cumul[:, :, None] - cumul[:, None, :]
    weights = jnp.where(causal, jnp.exp(jnp.where(causal, spread, 0.0)), 0.0)
    scores = (
        scale
        * jnp.einsum("thd,shd->hts", head_queries, head_keys, precision=lax.Precision.HIGHEST)
        * weights
    )
    pressure = (
        scale
        * jnp.einsum("thd,shd->hts", head_gradient, head_values, precision=lax.Precision.HIGHEST)
        * weights
    )
    grad_query = jnp.einsum("hts,shd->thd", pressure, head_keys, precision=lax.Precision.HIGHEST)
    grad_key = jnp.einsum("hts,thd->shd", pressure, head_queries, precision=lax.Precision.HIGHEST)
    grad_value = jnp.einsum("hts,thd->shd", scores, head_gradient, precision=lax.Precision.HIGHEST)
    ascending_decay = jnp.exp(cumul).T
    grad_query = grad_query + scale * ascending_decay[:, :, None] * jnp.einsum(
        "joy,oiy->joi", head_gradient, incoming_state, precision=lax.Precision.HIGHEST
    )
    state_update = jnp.einsum(
        "olb,oli->lbi",
        head_queries * ascending_decay[:, :, None],
        head_gradient,
        precision=lax.Precision.HIGHEST,
    )
    survive = jnp.exp(cumul[:, -1])
    falling = jnp.exp(cumul[:, -1:] - cumul).T
    return (grad_query, grad_key, grad_value, state_update, survive, falling)


def add_carried(grad_key, grad_value, head_keys, head_values, falling, carried_over_state):
    scale = head_keys.shape[-1] ** (-0.5)
    grad_key = grad_key + scale * falling[:, :, None] * jnp.einsum(
        "upy,ruy->rup", carried_over_state, head_values, precision=lax.Precision.HIGHEST
    )
    grad_value = grad_value + scale * falling[:, :, None] * jnp.einsum(
        "rzw,erz->erw", carried_over_state, head_keys, precision=lax.Precision.HIGHEST
    )
    return (grad_key, grad_value)


def body(
    mixer_out,
    layer_grad,
    row_scale,
    norm_gain,
    routes,
    route_weight,
    expert_gate,
    expert_up,
    expert_down,
    query_rows,
    key_rows,
    value_rows,
    retained,
    log_decay,
    entry_state,
    out_proj,
):
    experts = lax.axis_size("sp")
    tp_count = lax.axis_size("tp")
    tokens_here, columns = mixer_out.shape
    fanout = routes.shape[1]
    capacity = 2 * fanout * tokens_here // experts
    slots = experts * capacity
    chosen = routes[:, :, None] == jnp.arange(experts, dtype=jnp.int32)[None, None, :]
    counts = jnp.sum(chosen, axis=1).astype(BF16)
    places = jnp.arange(tokens_here)
    before = (places[:, None] > places[None, :]).astype(BF16)
    ranks = jnp.dot(before, counts, preferred_element_type=F32).astype(jnp.int32)
    rank_in = jnp.sum(jnp.where(chosen, ranks[:, None, :], 0), axis=2)
    slot_ids = routes * capacity + rank_in
    hits = slot_ids[:, :, None] == jnp.arange(slots, dtype=jnp.int32)[None, None, :]
    pick = jnp.any(hits, axis=1).astype(BF16)
    slot_weight = jnp.sum(jnp.where(hits, route_weight[:, :, None], 0.0), axis=(0, 1))
    gain_all = norm_gain.astype(F32)
    gain_cols = lax.dynamic_slice_in_dim(gain_all, lax.axis_index("tp") * columns, columns)
    scaled = mixer_out.astype(F32) * row_scale[:, None]
    normed = (scaled * gain_cols[None, :]).astype(BF16)
    send_normed = contract_first(pick, normed).astype(BF16).reshape(experts, capacity, columns)
    send_grad = (slot_weight[:, None] * contract_first(pick, layer_grad)).astype(BF16).reshape(
        experts, capacity, columns
    )
    normed_rows, grad_rows = dispatch(experts, tp_count, send_normed, send_grad)
    gate_weight = expert_gate[0]
    up_weight = expert_up[0]
    down_weight = expert_down[0]
    gate_pre = contract_last(normed_rows, gate_weight)
    up_pre = contract_last(normed_rows, up_weight)
    act_grad = contract_last(grad_rows, down_weight)
    sigmoid_gate = jax.nn.sigmoid(gate_pre)
    silu_gate = gate_pre * sigmoid_gate
    activation = (silu_gate * up_pre).astype(BF16)
    grad_down = contract_first(activation, grad_rows).astype(BF16)[None]
    up_grad = (act_grad * silu_gate).astype(BF16)
    gate_grad = (act_grad * up_pre * sigmoid_gate * (1.0 + gate_pre * (1.0 - sigmoid_gate))).astype(BF16)
    grad_up = contract_first(up_grad, normed_rows).astype(BF16)[None]
    partial_value = jnp.dot(gate_grad, gate_weight, preferred_element_type=F32) + jnp.dot(
        up_grad, up_weight, preferred_element_type=F32
    )
    head_count = entry_state.shape[1]
    head_dim = entry_state.shape[-1]
    survive_here = jnp.exp(jnp.sum(log_decay, axis=1))
    survive_tile = jnp.zeros((8, 128), F32).at[0, :head_count].set(survive_here)
    stream_grad, stream_full, kept_all, survive_all = give_back(
        experts,
        tp_count,
        partial_value.astype(BF16),
        pick,
        mixer_out,
        layer_grad,
        jnp.broadcast_to(row_scale[:, None], (tokens_here, 128)),
        gain_cols[None, :],
        retained,
        survive_tile,
    )
    out_grad = contract_last(stream_full, out_proj).astype(BF16)

    def split_heads(block):
        return block.astype(F32).reshape(tokens_here, head_count, head_dim)

    head_keys = split_heads(key_rows)
    head_values = split_heads(value_rows)
    grad_query, grad_key, grad_value, state_update, survive, falling = span_terms(
        split_heads(query_rows),
        head_keys,
        head_values,
        split_heads(out_grad),
        log_decay,
        entry_state[0],
    )
    spans = jnp.arange(experts)
    here = lax.axis_index("sp")
    between = (spans[None, :] > here) & (spans[None, :] < spans[:, None])
    factors = jnp.where(between[:, :, None], survive_all[None, :, 0, :head_count], 1.0)
    weight = jnp.prod(factors, axis=1) * (spans > here)[:, None]
    per_head = head_dim * head_dim // 128
    weight_rows = jnp.broadcast_to(
        weight[:, :, None, None], (experts, head_count, per_head, 128)
    ).reshape(experts, head_count * per_head, 128)
    cut = stream_full.reshape(tokens_here, experts, -1).transpose(1, 0, 2)
    carried, cols_all = exchange(
        experts, tp_count, state_update.astype(BF16).reshape(head_count * per_head, 128), weight_rows, cut
    )
    grad_key, grad_value = add_carried(
        grad_key, grad_value, head_keys, head_values, falling, carried.reshape(head_count, head_dim, head_dim)
    )
    grad_proj = contract_first(
        cols_all.reshape(-1, cols_all.shape[-1]), kept_all.reshape(-1, kept_all.shape[-1])
    )
    ret_cols = head_count * head_dim
    return (
        grad_up,
        grad_down,
        grad_proj,
        grad_query.reshape(tokens_here, ret_cols).astype(BF16),
        grad_key.reshape(tokens_here, ret_cols).astype(BF16),
        grad_value.reshape(tokens_here, ret_cols).astype(BF16),
        stream_grad,
    )


def solution(mesh):
    in_specs = (
        P("sp", "tp"),
        P("sp", "tp"),
        P("sp"),
        P(),
        P("sp", None),
        P("sp", None),
        P("sp", "tp", None),
        P("sp", "tp", None),
        P("sp", "tp", None),
        P("sp", "tp"),
        P("sp", "tp"),
        P("sp", "tp"),
        P("sp", "tp"),
        P("tp", "sp"),
        P("sp", "tp", None, None),
        P("tp", None),
    )
    out_specs = (
        P("sp", "tp", None),
        P("sp", "tp", None),
        P("sp", "tp"),
        P("sp", "tp"),
        P("sp", "tp"),
        P("sp", "tp"),
        P("sp", "tp"),
    )
    return jax.shard_map(body, mesh=mesh, in_specs=in_specs, out_specs=out_specs, check_vma=False)
```

```python
import functools
import math

import jax
import jax.numpy as jnp
from jax import lax
from jax.experimental import pallas as pl
from jax.experimental.pallas import tpu as pltpu
from jax.sharding import PartitionSpec as P

MESH = pl.DeviceIdType.MESH
VMEM = pl.BlockSpec(memory_space=pltpu.VMEM)
BF16, F32 = jnp.bfloat16, jnp.float32


def remote(src, dst, send_sem, recv_sem, device):
    return pltpu.make_async_remote_copy(
        src_ref=src, dst_ref=dst, send_sem=send_sem, recv_sem=recv_sem,
        device_id=device, device_id_type=MESH,
    )


def greet(devices):
    barrier = pltpu.get_barrier_semaphore()
    for device in devices:
        pl.semaphore_signal(barrier, inc=1, device_id=device, device_id_type=MESH)
    pl.semaphore_wait(barrier, len(devices))


class Place:
    def __init__(self, n, tp):
        self.n, self.tp, self.rows = n, tp, tp // 2
        self.s, self.t = lax.axis_index("sp"), lax.axis_index("tp")
        self.core, self.y = lax.rem(self.t, 2), self.t // 2
        self.twin_t = self.t + 1 - 2 * self.core
        self.twin = (self.s, self.twin_t)

    def to_sp(self, k):
        return lax.rem(self.s + k, self.n)

    def from_sp(self, k):
        return lax.rem(self.s + self.n - k, self.n)

    def to_y(self, k):
        return 2 * lax.rem(self.y + k, self.rows) + self.core

    def from_y(self, k):
        return 2 * lax.rem(self.y + self.rows - k, self.rows) + self.core

    def sp_peers(self):
        return [(self.to_sp(k), self.t) for k in range(1, self.n)]

    def tp_peers(self):
        return [(self.s, lax.rem(self.t + k, self.tp)) for k in range(1, self.tp)]

    def y_peers(self):
        return [(self.s, self.to_y(k)) for k in range(1, self.rows)] + [self.twin]


def dispatch_kernel(n, tp, normed_ref, grad_ref, gate_ref, up_ref, full_n_ref, full_g_ref, gate_pre_ref, up_pre_ref,
                    buf, held, wsem, s1, r1, s2, r2, s3, r3):
    at = Place(n, tp)
    capacity, columns = normed_ref.shape[1:]
    loads = [pltpu.make_async_copy(ref, held.at[i], wsem.at[i]) for i, ref in enumerate((gate_ref, up_ref))]
    for load in loads:
        load.start()
    greet(at.sp_peers() + at.y_peers())
    inputs = (normed_ref, grad_ref)
    pending = []

    def start(copy):
        copy.start()
        pending.append(copy)

    def spread(kind, source, block):
        for k in range(1, at.rows):
            start(remote(block, buf.at[kind, at.t, source], s2.at[kind, k - 1, source],
                         r2.at[kind, k - 1, source], (at.s, at.to_y(k))))
        start(remote(block, buf.at[kind, at.t, source], s3.at[kind, 0, source],
                     r3.at[kind, 0, source], at.twin))

    def hand_on(kind, source):
        for k in range(1, at.rows):
            slot = buf.at[kind, at.from_y(k), source]
            remote(slot, slot, s2.at[kind, k - 1, source], r2.at[kind, k - 1, source], at.twin).wait_recv()
            start(remote(slot, slot, s3.at[kind, k, source], r3.at[kind, k, source], at.twin))

    for kind in range(2):
        spread(kind, at.s, inputs[kind].at[at.s])
        for k in range(1, n):
            there = at.to_sp(k)
            start(remote(inputs[kind].at[there], buf.at[kind, at.t, at.s], s1.at[kind, there],
                         r1.at[kind, at.s], (there, at.t)))
        buf[kind, at.t, at.s] = inputs[kind][at.s]

    def complete(kind, out):
        for k in range(n):
            source = at.from_sp(k)
            for hop in range(at.rows):
                owner = at.twin_t if hop == 0 else lax.rem(at.from_y(hop) + 1 - 2 * at.core, tp)
                slot = buf.at[kind, owner, source]
                remote(slot, slot, s3.at[kind, hop, source], r3.at[kind, hop, source], at.twin).wait_recv()
        for t in range(tp):
            out[:, t * columns:(t + 1) * columns] = buf[kind, t].reshape(n * capacity, columns)

    hidden = gate_ref.shape[0]
    tile = math.gcd(hidden, 128)
    tiles = [(i, j) for j in range(hidden // tile) for i in range(2)]
    share = -(-len(tiles) // (n - 3))

    def work(count):
        for i, j in tiles[:count]:
            rows = slice(j * tile, (j + 1) * tile)
            (gate_pre_ref, up_pre_ref)[i][rows, :] = contract_last(held[i, rows, :], full_n_ref[...])
        del tiles[:count]

    lag = [(kind, at.s) for kind in range(2)]
    for kind in range(2):
        for k in range(1, n):
            source = at.from_sp(k)
            slot = buf.at[kind, at.t, source]
            remote(slot, slot, s1.at[kind, source], r1.at[kind, source], at.twin).wait_recv()
            spread(kind, source, slot)
            lag.append((kind, source))
            if len(lag) > 3:
                hand_on(*lag.pop(0))
            if kind == 1 and k == 3:
                complete(0, full_n_ref)
                for load in loads:
                    load.wait()
            if kind == 1 and k >= 3:
                work(share)
    for item in lag:
        hand_on(*item)
    work(len(tiles))
    complete(1, full_g_ref)
    for copy in pending:
        copy.wait_send()


def dispatch(n, tp, send_normed, send_grad, gate, up):
    _, capacity, columns = send_normed.shape
    rows = tp // 2
    full = jax.ShapeDtypeStruct((n * capacity, tp * columns), BF16)
    pre = jax.ShapeDtypeStruct((gate.shape[0], n * capacity), F32)
    dma = pltpu.SemaphoreType.DMA
    return pl.pallas_call(
        functools.partial(dispatch_kernel, n, tp),
        out_shape=(full, full, pre, pre),
        in_specs=[VMEM] * 2 + [pl.BlockSpec(memory_space=pl.ANY)] * 2,
        out_specs=(VMEM,) * 4,
        scratch_shapes=[
            pltpu.VMEM((2, tp, n, capacity, columns), BF16),
            pltpu.VMEM((2,) + gate.shape, BF16),
            dma((2,)),
            dma((2, n)), dma((2, n)),
            dma((2, rows, n)), dma((2, rows, n)),
            dma((2, rows, n)), dma((2, rows, n)),
        ],
        compiler_params=pltpu.CompilerParams(collective_id=1, has_side_effects=True),
        name="dispatch",
    )(send_normed, send_grad, gate, up)


def eye(size):
    return lax.broadcasted_iota(jnp.int32, (size, size), 0) == lax.broadcasted_iota(jnp.int32, (size, size), 1)


def return_kernel(n, tp, part_ref, pick_ref, mixer_ref, layer_ref, scale_ref, gain_ref, kept_ref, surv_ref,
                  act_ref, up_grad_ref, grad_rows_ref, normed_rows_ref,
                  stream_ref, full_ref, kept_all_ref, surv_all_ref, grad_down_ref, grad_up_ref,
                  b1, s1buf, b2, total, back, stat, sbuf,
                  sa, ra, sb, rb, sc, rc, sd, rd, se, re, sf, rf, sk, rk, sv, rv):
    at = Place(n, tp)
    tokens, columns = mixer_ref.shape
    capacity = back.shape[1]
    pair = at.s + 1 - 2 * lax.rem(at.s, 2)
    greet(at.sp_peers() + at.tp_peers())
    pending = []

    def start(copy):
        copy.start()
        pending.append(copy)

    for k in range(at.rows):
        yy = lax.rem(at.y + k, at.rows)
        cols = pl.ds(pl.multiple_of((2 * yy + 1 - at.core) * columns, 128), columns)
        start(remote(part_ref.at[:, cols], b1.at[yy], sa.at[yy], ra.at[yy], at.twin))
    for k in range(1, n):
        there = at.to_sp(k)
        start(remote(surv_ref, surv_all_ref.at[at.s], sv.at[there], rv.at[at.s], (there, at.t)))
    surv_all_ref[at.s] = surv_ref[...]
    for k in range(2, n, 2):
        there = at.to_sp(k)
        start(remote(kept_ref, kept_all_ref.at[at.s], sk.at[0, there], rk.at[at.s], (there, at.t)))
    start(remote(kept_ref, kept_all_ref.at[at.s], sk.at[1, at.s], rk.at[at.s], (pair, at.t)))
    kept_all_ref[at.s] = kept_ref[...]

    for k in range(at.rows):
        yy = lax.rem(at.y + k, at.rows)
        remote(b1.at[yy], b1.at[yy], sa.at[yy], ra.at[yy], at.twin).wait_recv()
    order = [at.to_sp(k) for k in range(1, n)] + [at.s]

    def rows_of(block):
        return pl.ds(pl.multiple_of(block * capacity, capacity), capacity)

    def mine(block, yy):
        cols = pl.ds(pl.multiple_of((2 * yy + at.core) * columns, 128), columns)
        return part_ref[rows_of(block), cols].astype(F32) + b1[yy, rows_of(block), :].astype(F32)

    for block in order:
        for k in range(1, at.rows):
            yy = lax.rem(at.y + k, at.rows)
            s1buf[k - 1, block] = mine(block, yy).astype(BF16)
            start(remote(s1buf.at[k - 1, block], b2.at[k - 1, block], sb.at[k - 1, block],
                         rb.at[k - 1, block], (at.s, at.to_y(k))))
    hidden_units = act_ref.shape[0]
    tile = math.gcd(hidden_units, 128)
    tiles = [(i, j) for i in range(2) for j in range(hidden_units // tile)]
    share = -(-len(tiles) // n)

    def work(count):
        for i, j in tiles[:count]:
            rows = slice(j * tile, (j + 1) * tile)
            left, right, out = (
                (act_ref, grad_rows_ref, grad_down_ref), (up_grad_ref, normed_rows_ref, grad_up_ref))[i]
            out[rows, :] = jnp.dot(left[rows, :], right[...], preferred_element_type=F32).astype(BF16)
        del tiles[:count]

    for place, block in enumerate(order):
        work(share)
        summed = mine(block, at.y)
        for k in range(1, at.rows):
            slot = b2.at[k - 1, block]
            remote(slot, slot, sb.at[k - 1, block], rb.at[k - 1, block], at.twin).wait_recv()
            summed = summed + b2[k - 1, block].astype(F32)
        if place < n - 1:
            total[block] = summed.astype(BF16)
            start(remote(total.at[block], back.at[at.s], sc.at[block], rc.at[at.s], (block, at.t)))
        else:
            back[at.s] = summed.astype(BF16)
    for k in range(2, n, 2):
        source = at.from_sp(k)
        slot = kept_all_ref.at[source]
        remote(slot, slot, sk.at[0, source], rk.at[source], at.twin).wait_recv()
        start(remote(slot, slot, sk.at[1, source], rk.at[source], (pair, at.t)))
    for k in range(1, n):
        source = at.from_sp(k)
        slot = back.at[source]
        remote(slot, slot, sc.at[source], rc.at[source], at.twin).wait_recv()
    hidden = jnp.dot(pick_ref[...], back[...].reshape(n * capacity, columns), preferred_element_type=F32)
    attend = gain_ref[...] * hidden.astype(BF16).astype(F32)
    row_scale = scale_ref[:, 0:1]
    scaled = mixer_ref[...].astype(F32) * row_scale
    column = jnp.sum(scaled * attend, axis=1, keepdims=True)
    diagonal = eye(tokens)
    row = jnp.sum(jnp.where(diagonal, column, 0.0), axis=0, keepdims=True)
    stat[at.t] = jnp.broadcast_to(row, (8, tokens))
    for k in range(1, tp):
        there = lax.rem(at.t + k, tp)
        start(remote(stat.at[at.t], stat.at[at.t], sd.at[there], rd.at[at.t], (at.s, there)))
    for k in range(1, tp):
        source = lax.rem(at.t + tp - k, tp)
        remote(stat.at[source], stat.at[source], sd.at[source], rd.at[source], at.twin).wait_recv()
    summed_row = jnp.sum(stat[...], axis=0)[0:1, :]
    mean_dot = jnp.sum(jnp.where(diagonal, summed_row, 0.0), axis=1, keepdims=True) / (columns * tp)
    stream = (layer_ref[...].astype(F32) + row_scale * (attend - scaled * mean_dot)).astype(BF16)
    stream_ref[...] = stream
    sbuf[at.t] = stream
    for k in range(1, at.rows):
        start(remote(sbuf.at[at.t], sbuf.at[at.t], se.at[k - 1], re.at[k - 1], (at.s, at.to_y(k))))
    start(remote(sbuf.at[at.t], sbuf.at[at.t], sf.at[0], rf.at[0], at.twin))
    for k in range(1, at.rows):
        slot = sbuf.at[at.from_y(k)]
        remote(slot, slot, se.at[k - 1], re.at[k - 1], at.twin).wait_recv()
        start(remote(slot, slot, sf.at[k], rf.at[k], at.twin))
    for hop in range(at.rows):
        owner = at.twin_t if hop == 0 else lax.rem(at.from_y(hop) + 1 - 2 * at.core, tp)
        slot = sbuf.at[owner]
        remote(slot, slot, sf.at[hop], rf.at[hop], at.twin).wait_recv()
    for t in range(tp):
        full_ref[:, t * columns:(t + 1) * columns] = sbuf[t]
    for k in range(1, n):
        source = at.from_sp(k)
        slot = surv_all_ref.at[source]
        remote(slot, slot, sv.at[source], rv.at[source], at.twin).wait_recv()
    for k in range(0, n, 2):
        source = lax.rem(pair + n - k, n)
        slot = kept_all_ref.at[source]
        remote(slot, slot, sk.at[0, source], rk.at[source], at.twin).wait_recv()
    for copy in pending:
        copy.wait_send()


def give_back(n, tp, part, pick, mixer, layer, row_scale, gain, kept, surv, act, up_grad, grad_rows, normed_rows):
    tokens, columns = mixer.shape
    rows, capacity = tp // 2, part.shape[0] // n
    dma = pltpu.SemaphoreType.DMA
    return pl.pallas_call(
        functools.partial(return_kernel, n, tp),
        out_shape=(
            jax.ShapeDtypeStruct((tokens, columns), BF16),
            jax.ShapeDtypeStruct((tokens, tp * columns), BF16),
            jax.ShapeDtypeStruct((n,) + kept.shape, BF16),
            jax.ShapeDtypeStruct((n,) + surv.shape, F32),
            jax.ShapeDtypeStruct((act.shape[0], tp * columns), BF16),
            jax.ShapeDtypeStruct((act.shape[0], tp * columns), BF16),
        ),
        in_specs=[VMEM] * 12,
        out_specs=(VMEM,) * 6,
        scratch_shapes=[
            pltpu.VMEM((rows, n * capacity, columns), BF16),
            pltpu.VMEM((rows, n, capacity, columns), BF16),
            pltpu.VMEM((rows, n, capacity, columns), BF16),
            pltpu.VMEM((n, capacity, columns), BF16),
            pltpu.VMEM((n, capacity, columns), BF16),
            pltpu.VMEM((tp, 8, tokens), F32),
            pltpu.VMEM((tp, tokens, columns), BF16),
            dma((rows,)), dma((rows,)),
            dma((rows, n)), dma((rows, n)),
            dma((n,)), dma((n,)),
            dma((tp,)), dma((tp,)),
            dma((rows,)), dma((rows,)),
            dma((rows,)), dma((rows,)),
            dma((2, n)), dma((n,)),
            dma((n,)), dma((n,)),
        ],
        compiler_params=pltpu.CompilerParams(collective_id=2, has_side_effects=True),
        name="give_back",
    )(part, pick, mixer, layer, row_scale, gain, kept, surv, act, up_grad, grad_rows, normed_rows)


def exchange_kernel(n, tp, state_ref, weight_ref, cut_ref, carried_ref, cols_ref, sbuf, cbuf, su, ru, sc, rc, sd, rd):
    at = Place(n, tp)
    tokens = cut_ref.shape[1]
    half = tokens // 2
    greet(at.sp_peers() + [at.twin])
    pending = []

    def start(copy):
        copy.start()
        pending.append(copy)

    own = pl.ds(pl.multiple_of(at.core * half, half), half)
    other = pl.ds(pl.multiple_of((1 - at.core) * half, half), half)
    for k in range(1, n):
        there = at.to_sp(k)
        start(remote(state_ref, sbuf.at[at.s], su.at[there], ru.at[at.s], (there, at.t)))
        start(remote(cut_ref.at[there, own], cbuf.at[at.s, own], sc.at[there], rc.at[at.s], (there, at.t)))
    sbuf[at.s] = state_ref[...]
    cbuf[at.s] = cut_ref[at.s]
    for k in range(1, n):
        source = at.from_sp(k)
        slot = cbuf.at[source, own]
        remote(slot, slot, sc.at[source], rc.at[source], at.twin).wait_recv()
        start(remote(slot, slot, sd.at[source], rd.at[source], at.twin))
    total = jnp.zeros(carried_ref.shape, F32)
    for k in range(1, n):
        source = at.from_sp(k)
        slot = sbuf.at[source]
        remote(slot, slot, su.at[source], ru.at[source], at.twin).wait_recv()
        total = total + weight_ref[source] * sbuf[source].astype(F32)
    carried_ref[...] = total
    for k in range(1, n):
        source = at.from_sp(k)
        slot = cbuf.at[source, other]
        remote(slot, slot, sd.at[source], rd.at[source], at.twin).wait_recv()
    cols_ref[...] = cbuf[...]
    for copy in pending:
        copy.wait_send()


def exchange(n, tp, state, weight, cut):
    dma = pltpu.SemaphoreType.DMA
    return pl.pallas_call(
        functools.partial(exchange_kernel, n, tp),
        out_shape=(jax.ShapeDtypeStruct(state.shape, F32), jax.ShapeDtypeStruct(cut.shape, BF16)),
        in_specs=[VMEM] * 3,
        out_specs=(VMEM, VMEM),
        scratch_shapes=[
            pltpu.VMEM((n,) + state.shape, BF16),
            pltpu.VMEM(cut.shape, BF16),
            dma((n,)), dma((n,)), dma((n,)), dma((n,)), dma((n,)), dma((n,)),
        ],
        compiler_params=pltpu.CompilerParams(collective_id=3, has_side_effects=True),
        name="exchange",
    )(state, weight, cut)


def contract_last(first_op, second_op):
    return lax.dot_general(
        first_op, second_op, (((1,), (1,)), ((), ())), preferred_element_type=jnp.float32
    )


def contract_first(first_op, second_op):
    return lax.dot_general(
        first_op, second_op, (((0,), (0,)), ((), ())), preferred_element_type=jnp.float32
    )


def span_terms(head_queries, head_keys, head_values, head_gradient, decay_head, incoming_state):
    scale = head_queries.shape[-1] ** (-0.5)
    length = decay_head.shape[1]
    cumul = jnp.cumsum(decay_head, axis=1)
    places = jnp.arange(length)
    causal = (places[:, None] >= places[None, :])[None, :, :]
    spread = cumul[:, :, None] - cumul[:, None, :]
    weights = jnp.where(causal, jnp.exp(jnp.where(causal, spread, 0.0)), 0.0)
    scores = (
        scale
        * jnp.einsum("thd,shd->hts", head_queries, head_keys, precision=lax.Precision.HIGHEST)
        * weights
    )
    pressure = (
        scale
        * jnp.einsum("thd,shd->hts", head_gradient, head_values, precision=lax.Precision.HIGHEST)
        * weights
    )
    grad_query = jnp.einsum("hts,shd->thd", pressure, head_keys, precision=lax.Precision.HIGHEST)
    grad_key = jnp.einsum("hts,thd->shd", pressure, head_queries, precision=lax.Precision.HIGHEST)
    grad_value = jnp.einsum("hts,thd->shd", scores, head_gradient, precision=lax.Precision.HIGHEST)
    ascending_decay = jnp.exp(cumul).T
    grad_query = grad_query + scale * ascending_decay[:, :, None] * jnp.einsum(
        "joy,oiy->joi", head_gradient, incoming_state, precision=lax.Precision.HIGHEST
    )
    state_update = jnp.einsum(
        "olb,oli->lbi",
        head_queries * ascending_decay[:, :, None],
        head_gradient,
        precision=lax.Precision.HIGHEST,
    )
    survive = jnp.exp(cumul[:, -1])
    falling = jnp.exp(cumul[:, -1:] - cumul).T
    return (grad_query, grad_key, grad_value, state_update, survive, falling)


def add_carried(grad_key, grad_value, head_keys, head_values, falling, carried_over_state):
    scale = head_keys.shape[-1] ** (-0.5)
    grad_key = grad_key + scale * falling[:, :, None] * jnp.einsum(
        "upy,ruy->rup", carried_over_state, head_values, precision=lax.Precision.HIGHEST
    )
    grad_value = grad_value + scale * falling[:, :, None] * jnp.einsum(
        "rzw,erz->erw", carried_over_state, head_keys, precision=lax.Precision.HIGHEST
    )
    return (grad_key, grad_value)


def body(
    mixer_out,
    layer_grad,
    row_scale,
    norm_gain,
    routes,
    route_weight,
    expert_gate,
    expert_up,
    expert_down,
    query_rows,
    key_rows,
    value_rows,
    retained,
    log_decay,
    entry_state,
    out_proj,
):
    experts = lax.axis_size("sp")
    tp_count = lax.axis_size("tp")
    tokens_here, columns = mixer_out.shape
    fanout = routes.shape[1]
    capacity = 2 * fanout * tokens_here // experts
    slots = experts * capacity
    chosen = routes[:, :, None] == jnp.arange(experts, dtype=jnp.int32)[None, None, :]
    counts = jnp.sum(chosen, axis=1).astype(BF16)
    places = jnp.arange(tokens_here)
    before = (places[:, None] > places[None, :]).astype(BF16)
    ranks = jnp.dot(before, counts, preferred_element_type=F32).astype(jnp.int32)
    rank_in = jnp.sum(jnp.where(chosen, ranks[:, None, :], 0), axis=2)
    slot_ids = routes * capacity + rank_in
    hits = slot_ids[:, :, None] == jnp.arange(slots, dtype=jnp.int32)[None, None, :]
    pick = jnp.any(hits, axis=1).astype(BF16)
    slot_weight = jnp.sum(jnp.where(hits, route_weight[:, :, None], 0.0), axis=(0, 1))
    gain_all = norm_gain.astype(F32)
    gain_cols = lax.dynamic_slice_in_dim(gain_all, lax.axis_index("tp") * columns, columns)
    scaled = mixer_out.astype(F32) * row_scale[:, None]
    normed = (scaled * gain_cols[None, :]).astype(BF16)
    send_normed = contract_first(pick, normed).astype(BF16).reshape(experts, capacity, columns)
    send_grad = (slot_weight[:, None] * contract_first(pick, layer_grad)).astype(BF16).reshape(
        experts, capacity, columns
    )
    gate_weight = expert_gate[0]
    up_weight = expert_up[0]
    down_weight = expert_down[0]
    normed_rows, grad_rows, gate_pre, up_pre = dispatch(
        experts, tp_count, send_normed, send_grad, gate_weight, up_weight
    )
    act_grad = contract_last(down_weight, grad_rows)
    sigmoid_gate = jax.nn.sigmoid(gate_pre)
    silu_gate = gate_pre * sigmoid_gate
    activation = (silu_gate * up_pre).astype(BF16)
    up_grad = (act_grad * silu_gate).astype(BF16)
    gate_grad = (act_grad * up_pre * sigmoid_gate * (1.0 + gate_pre * (1.0 - sigmoid_gate))).astype(BF16)
    partial_value = contract_first(gate_grad, gate_weight) + contract_first(up_grad, up_weight)
    head_count = entry_state.shape[1]
    head_dim = entry_state.shape[-1]
    survive_here = jnp.exp(jnp.sum(log_decay, axis=1))
    survive_tile = jnp.zeros((8, 128), F32).at[0, :head_count].set(survive_here)
    stream_grad, stream_full, kept_all, survive_all, grad_down, grad_up = give_back(
        experts,
        tp_count,
        partial_value.astype(BF16),
        pick,
        mixer_out,
        layer_grad,
        jnp.broadcast_to(row_scale[:, None], (tokens_here, 128)),
        gain_cols[None, :],
        retained,
        survive_tile,
        activation,
        up_grad,
        grad_rows,
        normed_rows,
    )
    out_grad = contract_last(stream_full, out_proj).astype(BF16)

    def split_heads(block):
        return block.astype(F32).reshape(tokens_here, head_count, head_dim)

    head_keys = split_heads(key_rows)
    head_values = split_heads(value_rows)
    grad_query, grad_key, grad_value, state_update, survive, falling = span_terms(
        split_heads(query_rows),
        head_keys,
        head_values,
        split_heads(out_grad),
        log_decay,
        entry_state[0],
    )
    spans = jnp.arange(experts)
    here = lax.axis_index("sp")
    between = (spans[None, :] > here) & (spans[None, :] < spans[:, None])
    factors = jnp.where(between[:, :, None], survive_all[None, :, 0, :head_count], 1.0)
    weight = jnp.prod(factors, axis=1) * (spans > here)[:, None]
    per_head = head_dim * head_dim // 128
    weight_rows = jnp.broadcast_to(
        weight[:, :, None, None], (experts, head_count, per_head, 128)
    ).reshape(experts, head_count * per_head, 128)
    cut = stream_full.reshape(tokens_here, experts, -1).transpose(1, 0, 2)
    carried, cols_all = exchange(
        experts, tp_count, state_update.astype(BF16).reshape(head_count * per_head, 128), weight_rows, cut
    )
    grad_key, grad_value = add_carried(
        grad_key, grad_value, head_keys, head_values, falling, carried.reshape(head_count, head_dim, head_dim)
    )
    grad_proj = contract_first(
        cols_all.reshape(-1, cols_all.shape[-1]), kept_all.reshape(-1, kept_all.shape[-1])
    )
    ret_cols = head_count * head_dim
    return (
        grad_up[None],
        grad_down[None],
        grad_proj,
        grad_query.reshape(tokens_here, ret_cols).astype(BF16),
        grad_key.reshape(tokens_here, ret_cols).astype(BF16),
        grad_value.reshape(tokens_here, ret_cols).astype(BF16),
        stream_grad,
    )


def solution(mesh):
    in_specs = (
        P("sp", "tp"),
        P("sp", "tp"),
        P("sp"),
        P(),
        P("sp", None),
        P("sp", None),
        P("sp", "tp", None),
        P("sp", "tp", None),
        P("sp", "tp", None),
        P("sp", "tp"),
        P("sp", "tp"),
        P("sp", "tp"),
        P("sp", "tp"),
        P("tp", "sp"),
        P("sp", "tp", None, None),
        P("tp", None),
    )
    out_specs = (
        P("sp", "tp", None),
        P("sp", "tp", None),
        P("sp", "tp"),
        P("sp", "tp"),
        P("sp", "tp"),
        P("sp", "tp"),
        P("sp", "tp"),
    )
    return jax.shard_map(body, mesh=mesh, in_specs=in_specs, out_specs=out_specs, check_vma=False)
```
